512 devices in a mesh: ep: 32 (over z, x), tp: 16 (over y, core).
Axes of the slice: x: 4, y: 8, z: 8, core: 2. Of those that a mesh axis runs over, the one named last changes fastest.
Arguments:
- queries: bfloat16 [4096, 512], P('ep'), may hold values from -6 to 6
- key_vectors: bfloat16 [4096, 512], P('ep'), may hold values from -6 to 6
- values: bfloat16 [4096, 1024], P('ep', 'tp'), may hold values from -6 to 6
- out_gate: bfloat16 [4096, 1024], P('ep', 'tp'), may hold values from -6 to 6
- input_gate: float32 [4096, 2], P('ep'), may hold values from -8 to 130
- forget_gate: float32 [4096, 2], P('ep'), may hold values from -2 to 16
- mix_weight: bfloat16 [1024, 2048], P('tp'), may hold values from -0.1875 to 0.1875
- expert_input: bfloat16 [8192, 2048], P('ep'), may hold values from -6 to 6
- norm_gain: float32 [2048], replicated, may hold values from 0.1 to 1.9
- route_ids: int32 [8192, 4], P('ep'), may hold values from 0 to 63, all different within a row; in each aligned block of 256 rows (0 to 255, 256 to 511, ...) at most 32 rows name the same one
- route_weights: float32 [8192, 4], P('ep'), may hold values from 0.2 to 1.2
- expert_gate: bfloat16 [512, 2048, 128], P(('ep', 'tp')), may hold values from -0.125 to 0.125
- expert_up: bfloat16 [512, 2048, 128], P(('ep', 'tp')), may hold values from -0.125 to 0.125
- expert_down: bfloat16 [512, 128, 2048], P(('ep', 'tp')), may hold values from -0.1875 to 0.1875
- shared_gate: bfloat16 [2048, 512], P(None, 'tp'), may hold values from -0.125 to 0.125
- shared_up: bfloat16 [2048, 512], P(None, 'tp'), may hold values from -0.125 to 0.125
- shared_down: bfloat16 [512, 2048], P('tp'), may hold values from -0.25 to 0.25
Outputs:
- mixer_out: bfloat16 [4096, 2048], P('ep')
- expert_out: bfloat16 [8192, 2048], P('ep')
The draws below stay inside these ranges and needn't reach their ends.
Inputs may be any that keep to these rules, and one draw needn't show every extreme that they name: `route_ids`: each row names 4 different experts. In each aligned block of 256 rows (the rows of one index of ep) no expert is named by more than 32 rows, and in some block one expert is named by exactly 32 rows.
All inputs are finite; a program needn't handle non-finite values.
Results may differ from the reference program's by a relative error of at most 0.01575.
Values may be sent and summed in bfloat16 or wider, within the bound.
A program may use at most 64 MiB of HBM per device.

```python
import math
import jax
import jax.numpy as jnp
import numpy as np
from jax import lax

D = 2048
MEMORY_HEADS = 2
KEY_DIM = 256
VAL_DIM = 512
BLOCK = 128
MOE_DEV = 256
TOPK = 4
FF = 1024
FF_SHARED = 512
MIXER_TOKEN_COUNT = 4096
MOE_TOKENS = 8192
TP_GROUP = 8
FF_DEV = 128
EXPERTS = 64
CAP = 32
VAL_DEV = 64
N_EP = 32
N_TP = 16


def draw_input_gate(key, part):
    random_subkeys = jax.random.split(jax.random.fold_in(key, 23), 1)
    pre_gate = jnp.clip(1.5 * jax.random.normal(random_subkeys[0], (MIXER_TOKEN_COUNT, MEMORY_HEADS), jnp.float32), -7.5, 7.5)
    return pre_gate


def draw_forget_gate(key, part):
    random_subkeys = jax.random.split(jax.random.fold_in(key, 41), 5)
    token_positions = jnp.arange(MIXER_TOKEN_COUNT, dtype=jnp.int32)
    shuffled = jax.random.permutation(random_subkeys[0], MEMORY_HEADS)
    slow_heads = (shuffled < MEMORY_HEADS // 2).astype(jnp.float32)
    slow_rate = 0.5
    baseline_rate = slow_heads * (slow_rate / MIXER_TOKEN_COUNT) + (1.0 - slow_heads) / 40.0
    block_multiplier = jnp.exp(jax.random.uniform(random_subkeys[1], (MIXER_TOKEN_COUNT // BLOCK, MEMORY_HEADS), jnp.float32, -0.69, 0.69))
    block_multiplier = jnp.repeat(block_multiplier, BLOCK, axis=0)
    jitter_amount = jnp.exp(jax.random.uniform(random_subkeys[2], (MIXER_TOKEN_COUNT, MEMORY_HEADS), jnp.float32, -1.1, 1.1))
    spike_position = jax.random.randint(random_subkeys[3], (3, MEMORY_HEADS), 0, MIXER_TOKEN_COUNT)
    spike_flag = jnp.any(token_positions[:, None, None] == spike_position[None, :, :], axis=1)
    spike_magnitude = jnp.log(jax.random.uniform(random_subkeys[4], (MIXER_TOKEN_COUNT, MEMORY_HEADS), jnp.float32, 0.5, 0.8))
    log_retention = -baseline_rate[None, :] * block_multiplier * jitter_amount + jnp.where(spike_flag, spike_magnitude, 0.0)
    return log_retention - jnp.log(-jnp.expm1(log_retention))


def levels(stream_key, dims, shards, least, high):
    def one(dim, shards_of):
        steps = jax.random.uniform(jax.random.fold_in(jax.random.fold_in(stream_key, 6), dim), (shards_of,), jnp.float32, least / len(shards), high / len(shards))
        return jnp.repeat(jnp.exp(steps), dims[dim] // shards_of).reshape((-1,) + (1,) * (len(dims) - dim - 1))

    factor_of = one(*shards[0])
    for cut in shards[1:]:
        factor_of = factor_of * one(*cut)
    return factor_of


def deal_out(stream_key, own, number, rows, count, top, limit, lean):
    order = jax.random.permutation(stream_key, count)
    crowded, ordinary = shares(count, rows * top, limit, lean, True), shares(count, rows * top, limit, lean, False)
    places = jnp.arange(count)

    def named(tallies, rotation):
        used = int((tallies > 0).sum())
        fixed = max(1, used // 4)
        shifted = fixed + (places - fixed + rotation * (used - fixed)) % max(1, count - fixed)
        return jnp.zeros((count,), jnp.int32).at[order[jnp.where(places < fixed, places, shifted)]].set(jnp.asarray(tallies, jnp.int32))

    tallies = jnp.where(number % 4 == 0, named(crowded, number // 4), named(ordinary, number - number // 4 - 1))
    mixed = jax.random.permutation(jax.random.fold_in(own, 3), count)
    donor, sink = mixed[0:count // 2 * 2:2], mixed[1:count // 2 * 2:2]
    margin = jnp.minimum(tallies[donor] - 1, limit - tallies[sink]) // 2
    margin = jnp.where((donor == order[0]) | (sink == order[0]) | (tallies[sink] == 0), 0, jnp.maximum(margin, 0))
    shifted = jax.random.randint(jax.random.fold_in(own, 4), (count // 2,), 0, 1 << 20) % (margin + 1)
    tallies = tallies.at[donor].add(-shifted).at[sink].add(shifted)
    members = jnp.searchsorted(jnp.cumsum(tallies), jnp.arange(rows * top), side="right").astype(jnp.int32)
    grid = members.reshape(top, rows).T
    grid = grid[jax.random.permutation(jax.random.fold_in(own, 1), rows)]
    rotation = jax.random.randint(jax.random.fold_in(own, 2), (rows, 1), 0, top)
    return jnp.take_along_axis(grid, (jnp.arange(top)[None, :] + rotation) % top, axis=1)


def shares(count, total, limit, skew, full):
    weights = [(1 << 20) // math.isqrt(standing ** skew) + 1 for standing in range(1, count + 1)]
    largest = limit if full else min(limit, max(-(-total // count), total * weights[0] // sum(weights)))
    least = 1 if total - largest >= count - 1 else 0
    given, rest = [largest] + [least] * (count - 1), total - largest - least * (count - 1)
    while rest > 0:
        free = [i for i in range(1, count) if given[i] < largest] or [i for i in range(1, count) if given[i] < limit]
        pool, left = sum([weights[i] for i in free]), rest
        for i in free:
            extra = min(limit - given[i], max(1, left * weights[i] // pool), rest)
            given[i] = given[i] + extra
            rest = rest - extra
    return np.array(given)


def centred(rng, shape, width, reach, shards=(), held_as=jnp.bfloat16):
    entries = width * jax.random.normal(rng, shape, jnp.float32)
    if shards:
        entries = entries * levels(rng, shape, shards, -0.22, 0.18)
    return jnp.clip(entries, -reach, reach).astype(held_as)


def setup_inputs(seed: int = 0) -> dict:
    keys = jax.random.split(jax.random.key(seed), 18)
    queries = centred(keys[0], (MIXER_TOKEN_COUNT, MEMORY_HEADS * KEY_DIM), 1.0, 6.0, ((0, 32),))
    key_vectors = centred(keys[1], (MIXER_TOKEN_COUNT, MEMORY_HEADS * KEY_DIM), 1.0, 6.0, ((0, 32),))
    values = centred(keys[2], (MIXER_TOKEN_COUNT, MEMORY_HEADS * VAL_DIM), 1.0, 6.0, ((0, 32), (1, 16)))
    out_gate = centred(keys[3], (MIXER_TOKEN_COUNT, MEMORY_HEADS * VAL_DIM), 1.0, 6.0, ((0, 32), (1, 16)))
    input_gate = draw_input_gate(jax.random.fold_in(keys[17], 71), 0)
    forget_gate = draw_forget_gate(jax.random.fold_in(keys[17], 71), 0)
    mix_weight = centred(keys[6], (MEMORY_HEADS * VAL_DIM, D), (MEMORY_HEADS * VAL_DIM) ** -0.5, 0.1875, ((0, 16),))
    expert_input = centred(keys[7], (MOE_TOKENS, D), 1.0, 6.0, ((0, 32),))
    norm_gain = jnp.clip(1.0 + 0.18 * jax.random.normal(keys[8], (D,), jnp.float32), 0.1, 1.9)
    route_ids_keys = jax.random.split(jax.random.fold_in(keys[9], 1), MOE_TOKENS // MOE_DEV)
    route_ids_turns = jax.random.permutation(jax.random.fold_in(keys[9], 3), MOE_TOKENS // MOE_DEV)
    route_ids = jax.vmap(lambda own, number: deal_out(jax.random.fold_in(keys[9], 2), own, number, MOE_DEV, EXPERTS, TOPK, CAP, 2))(route_ids_keys, route_ids_turns).reshape((MOE_TOKENS, TOPK))
    route_weights = jnp.clip(0.2 + 1 * jax.random.uniform(keys[10], (MOE_TOKENS, TOPK), jnp.float32) ** levels(keys[10], (MOE_TOKENS, TOPK), ((0, 32),), -0.2, 0.2), 0.2, 1.2)
    expert_gate = centred(keys[11], (EXPERTS * TP_GROUP, D, FF_DEV), D ** -0.5, 0.125, ((0, 512),))
    expert_up = centred(keys[12], (EXPERTS * TP_GROUP, D, FF_DEV), D ** -0.5, 0.125, ((0, 512),))
    expert_down = centred(keys[13], (EXPERTS * TP_GROUP, FF_DEV, D), FF ** -0.5, 0.1875, ((0, 512),))
    shared_gate = centred(keys[14], (D, FF_SHARED), D ** -0.5, 0.125, ((1, 16),))
    shared_up = centred(keys[15], (D, FF_SHARED), D ** -0.5, 0.125, ((1, 16),))
    shared_down = centred(keys[16], (FF_SHARED, D), FF_SHARED ** -0.5, 0.25, ((0, 16),))
    return dict(queries=queries, key_vectors=key_vectors, values=values, out_gate=out_gate, input_gate=input_gate, forget_gate=forget_gate, mix_weight=mix_weight, expert_input=expert_input, norm_gain=norm_gain, route_ids=route_ids, route_weights=route_weights, expert_gate=expert_gate, expert_up=expert_up, expert_down=expert_down, shared_gate=shared_gate, shared_up=shared_up, shared_down=shared_down)


epsilon = 1e-06
den_floor = 4.0

def mixer_part(queries, key_vectors, values, out_gate, input_gate, forget_gate, mix_weight):
    length = queries.shape[0]
    blocks = length // BLOCK
    factor = KEY_DIM ** (-0.5)
    causal = jnp.tril(jnp.ones((BLOCK, BLOCK), dtype=bool))

    def by_head(matrix, columns):
        return matrix.reshape(blocks, BLOCK, MEMORY_HEADS, columns).transpose(0, 2, 1, 3)
    query_blocks = by_head(queries, KEY_DIM)
    key_blocks = by_head(key_vectors, KEY_DIM)
    value_blocks = by_head(values, VAL_DIM)
    input_blocks = input_gate.reshape(blocks, BLOCK, MEMORY_HEADS).transpose(0, 2, 1)
    forget_blocks = jax.nn.log_sigmoid(forget_gate).reshape(blocks, BLOCK, MEMORY_HEADS).transpose(0, 2, 1)

    def block_step(carry_in, inputs):
        memory, normalizer, running = carry_in
        query_block, key_block, value_block, input_block, forget_block = inputs
        cumulative = jnp.cumsum(forget_block, axis=-1)
        carried = cumulative + running[:, None]
        log_weight = cumulative[:, :, None] - cumulative[:, None, :] + input_block[:, None, :]
        log_weight = jnp.where(causal, log_weight, -jnp.inf)
        stabilizer = jnp.maximum(carried, lax.optimization_barrier(jnp.max(log_weight, axis=-1)))
        within = jnp.exp(log_weight - stabilizer[:, :, None])
        across = jnp.exp(carried - stabilizer)
        query_wide = query_block.astype(jnp.float32)
        key_wide = key_block.astype(jnp.float32)
        value_wide = value_block.astype(jnp.float32)
        scores = jnp.einsum('htd,hsd->hts', query_wide, key_wide) * factor
        weights = scores * within
        weights_low = lax.optimization_barrier(weights.astype(jnp.bfloat16)).astype(jnp.float32)
        scaled = query_wide * factor
        numerator = across[:, :, None] * jnp.einsum('htd,hdv->htv', scaled, memory, precision=lax.Precision.HIGHEST)
        numerator = numerator + jnp.einsum('hts,hsv->htv', weights_low, value_wide)
        denominator = across * jnp.einsum('htd,hd->ht', scaled, normalizer, precision=lax.Precision.HIGHEST)
        denominator = denominator + lax.optimization_barrier(jnp.sum(weights, axis=-1))
        hidden = numerator / jnp.maximum(jnp.abs(denominator), den_floor)[:, :, None]
        block_total = cumulative[:, -1]
        log_retention = block_total[:, None] - cumulative + input_block
        running_next = jnp.maximum(block_total + running, lax.optimization_barrier(jnp.max(log_retention, axis=-1)))
        carry_decay = jnp.exp(block_total + running - running_next)
        weighted_keys = key_wide * jnp.exp(log_retention - running_next[:, None])[:, :, None]
        memory = carry_decay[:, None, None] * memory + jnp.einsum('hsd,hsv->hdv', weighted_keys, value_wide, precision=lax.Precision.HIGHEST)
        normalizer = carry_decay[:, None] * normalizer + lax.optimization_barrier(jnp.sum(weighted_keys, axis=1))
        return ((memory, normalizer, running_next), hidden)
    initial = (jnp.zeros((MEMORY_HEADS, KEY_DIM, VAL_DIM), jnp.float32), jnp.zeros((MEMORY_HEADS, KEY_DIM), jnp.float32), jnp.zeros((MEMORY_HEADS,), jnp.float32))
    _, hidden = lax.scan(block_step, initial, (query_blocks, key_blocks, value_blocks, input_blocks, forget_blocks))
    hidden = hidden.transpose(0, 2, 1, 3).reshape(length, MEMORY_HEADS * VAL_DIM)
    gated_rows = (hidden * jax.nn.sigmoid(out_gate.astype(jnp.float32))).astype(jnp.bfloat16)

    def add_group(summed, group_index):
        offset = (group_index * VAL_DEV).astype(jnp.int32)
        partial_value = jnp.dot(lax.dynamic_slice_in_dim(gated_rows, offset, VAL_DEV, 1), lax.dynamic_slice_in_dim(mix_weight, offset, VAL_DEV, 0), preferred_element_type=jnp.float32)
        return (summed + lax.optimization_barrier(partial_value.astype(jnp.bfloat16)).astype(jnp.float32), None)
    summed, _ = lax.scan(add_group, jnp.zeros((length, D), jnp.float32), jnp.arange(N_TP, dtype=jnp.int32))
    return summed.astype(jnp.bfloat16)

def expert_part(expert_input, norm_gain, route_ids, route_weights, expert_gate, expert_up, expert_down, shared_gate, shared_up, shared_down):
    rows_wide = expert_input.astype(jnp.float32)
    normed = (rows_wide * lax.rsqrt(lax.optimization_barrier(jnp.mean(rows_wide * rows_wide, axis=-1, keepdims=True)) + epsilon) * norm_gain).astype(jnp.bfloat16)
    chosen = route_ids.reshape(N_EP, MOE_DEV * TOPK)
    onehot = (chosen[:, :, None] == jnp.arange(EXPERTS, dtype=jnp.int32)[None, None, :]).astype(jnp.int32)
    earlier = jnp.cumsum(onehot, axis=1) - onehot
    slot_rank = lax.optimization_barrier(jnp.sum(earlier * onehot, axis=2))
    slot_index = (jnp.arange(N_EP, dtype=jnp.int32)[:, None] * CAP + slot_rank).reshape(-1)
    expert_of = route_ids.reshape(-1)
    token_of = jnp.arange(MOE_TOKENS * TOPK, dtype=jnp.int32) // TOPK
    slot_token = jnp.zeros((EXPERTS, N_EP * CAP), jnp.int32).at[expert_of, slot_index].set(token_of)
    slot_weight = jnp.zeros((EXPERTS, N_EP * CAP), jnp.float32).at[expert_of, slot_index].set(route_weights.reshape(-1))

    def one_expert(routed, expert_index):
        tokens_here = slot_token[expert_index]
        weight_here = slot_weight[expert_index]
        picked = normed[tokens_here].astype(jnp.float32)
        rows_base = (expert_index * TP_GROUP).astype(jnp.int32)
        gate_w = lax.dynamic_slice_in_dim(expert_gate, rows_base, TP_GROUP, 0).astype(jnp.float32)
        up_w = lax.dynamic_slice_in_dim(expert_up, rows_base, TP_GROUP, 0).astype(jnp.float32)
        down_w = lax.dynamic_slice_in_dim(expert_down, rows_base, TP_GROUP, 0).astype(jnp.float32)
        gate_val = jnp.einsum('rd,gdf->rgf', picked, gate_w)
        up_val = jnp.einsum('rd,gdf->rgf', picked, up_w)
        hidden = lax.optimization_barrier((jax.nn.silu(gate_val) * up_val).astype(jnp.bfloat16)).astype(jnp.float32)
        partials = jnp.einsum('rgf,gfd->rgd', hidden, down_w)
        partials = lax.optimization_barrier(partials.astype(jnp.bfloat16)).astype(jnp.float32)
        result = lax.optimization_barrier(jnp.sum(partials, axis=1)) * weight_here[:, None]
        return (routed.at[tokens_here].add(result), None)
    routed, _ = lax.scan(one_expert, jnp.zeros((MOE_TOKENS, D), jnp.float32), jnp.arange(EXPERTS, dtype=jnp.int32))
    shared_gate_val = jnp.dot(normed, shared_gate, preferred_element_type=jnp.float32)
    shared_up_val = jnp.dot(normed, shared_up, preferred_element_type=jnp.float32)
    shared_act = (jax.nn.silu(shared_gate_val) * shared_up_val).astype(jnp.bfloat16)
    shared_rows = jnp.dot(shared_act, shared_down, preferred_element_type=jnp.float32)
    return (routed + shared_rows).astype(jnp.bfloat16)

def reference(queries, key_vectors, values, out_gate, input_gate, forget_gate, mix_weight, expert_input, norm_gain, route_ids, route_weights, expert_gate, expert_up, expert_down, shared_gate, shared_up, shared_down):
    mixer_out = mixer_part(queries, key_vectors, values, out_gate, input_gate, forget_gate, mix_weight)
    expert_out = expert_part(expert_input, norm_gain, route_ids, route_weights, expert_gate, expert_up, expert_down, shared_gate, shared_up, shared_down)
    return (mixer_out, expert_out)
```

```python
import functools

import jax
import jax.numpy as jnp
from jax import lax
from jax.experimental import pallas as pl
from jax.experimental.pallas import tpu as pltpu
from jax.sharding import Mesh
from jax.sharding import PartitionSpec as P

MEMORY_HEADS = 2
KEY_DIM = 256
CAP = 32
ROWS = CAP // 2
LANES = 128
EP = ("z", "x")
TP = ("y", "c")
MESH = pl.DeviceIdType.MESH

epsilon = 1e-06
lowest = -1e30
den_floor = 4.0


def mixer_local(queries, key_vectors, values, out_gate, input_gate, forget_gate, head):
    length = queries.shape[0]
    factor = KEY_DIM ** (-0.5)
    offset = head * KEY_DIM
    query = lax.dynamic_slice_in_dim(queries, offset, KEY_DIM, 1)
    key = lax.dynamic_slice_in_dim(key_vectors, offset, KEY_DIM, 1)
    select = jnp.arange(MEMORY_HEADS, dtype=jnp.int32)[None, :] == head
    gate_in = jnp.sum(jnp.where(select, input_gate, 0.0), axis=1)
    lf = jax.nn.log_sigmoid(jnp.sum(jnp.where(select, forget_gate, 0.0), axis=1))
    causal = jnp.tril(jnp.ones((length, length), dtype=bool))
    cumulative = jnp.sum(jnp.where(causal, lf[None, :], 0.0), axis=1)
    total = cumulative[length - 1]
    log_keep = total - cumulative + gate_in
    running = jnp.max(log_keep)
    weighted = key.astype(jnp.float32) * jnp.exp(log_keep - running)[:, None]
    memory_t = lax.dot_general(
        values.astype(jnp.float32),
        weighted,
        (((0,), (0,)), ((), ())),
        precision=lax.Precision.HIGHEST,
    )
    stats = jnp.concatenate(
        [
            jnp.sum(weighted, axis=0)[None, :],
            jnp.broadcast_to(total, (1, KEY_DIM)),
            jnp.broadcast_to(running, (1, KEY_DIM)),
            jnp.zeros((5, KEY_DIM), jnp.float32),
        ]
    )
    state = jnp.concatenate([memory_t, stats])
    log_weight = cumulative[:, None] - cumulative[None, :] + gate_in[None, :]
    log_weight = jnp.where(causal, log_weight, -jnp.inf)
    peak = jnp.max(log_weight, axis=1)
    scores = (
        lax.dot_general(
            query, key, (((1,), (1,)), ((), ())), preferred_element_type=jnp.float32
        )
        * factor
    )
    weights = scores * jnp.exp(log_weight - peak[:, None])
    inside_t = lax.dot_general(
        values,
        weights.astype(jnp.bfloat16),
        (((0,), (1,)), ((), ())),
        preferred_element_type=jnp.float32,
    )
    rows = jnp.concatenate(
        [
            cumulative[None, :],
            peak[None, :],
            jnp.sum(weights, axis=1)[None, :],
            jnp.zeros((5, length), jnp.float32),
        ]
    )
    gate_t = jax.nn.sigmoid(out_gate.astype(jnp.float32)).T
    scaled = query * jnp.asarray(factor, jnp.bfloat16)
    return state, rows, inside_t, gate_t, scaled


def routing(route_ids, route_weights, team, core, nz, nx):
    tokens, top = route_ids.shape
    count = nz * nx
    wanted = jnp.arange(count, dtype=jnp.int32)[None, :] * 2 + team
    named = jnp.zeros((tokens, count), jnp.float32)
    weight = jnp.zeros((tokens, count), jnp.float32)
    for k in range(top):
        hit = route_ids[:, k : k + 1] == wanted
        named = named + hit.astype(jnp.float32)
        weight = weight + jnp.where(hit, route_weights[:, k : k + 1], 0.0)
    earlier = jnp.tril(jnp.ones((tokens, tokens), jnp.bfloat16), -1)
    rank = jnp.dot(earlier, named.astype(jnp.bfloat16), preferred_element_type=jnp.float32)
    slot = jnp.where(named > 0, rank, -1.0).astype(jnp.int32) - core * ROWS
    by_dest = slot.reshape(tokens, nz, nx).transpose(2, 1, 0)
    weight_by = weight.reshape(tokens, nz, nx).transpose(2, 1, 0)
    own = jnp.arange(ROWS, dtype=jnp.int32)[None, None, :, None]
    hit = by_dest[:, :, None, :] == own
    pick = hit.astype(jnp.bfloat16).reshape(nx, nz * ROWS, tokens)
    spread = jnp.where(hit, weight_by[:, :, None, :], 0.0)
    high = lax.reduce_precision(spread, 8, 7)
    low = spread - high
    high = high.astype(jnp.bfloat16).reshape(nx, nz * ROWS, tokens)
    low = low.astype(jnp.bfloat16).reshape(nx, nz * ROWS, tokens)
    return pick, high, low


def kernel(
    nz,
    nx,
    ny,
    xh,
    pick,
    whi,
    wlo,
    gate_in,
    up_in,
    down_in,
    state,
    rows,
    inside,
    sig,
    scaled,
    mixw,
    act_in,
    shdown,
    mixer_out,
    expert_out,
    gate,
    up,
    down,
    disp,
    xown,
    xnbr,
    pkeep,
    psend,
    precv,
    back,
    rbuf,
    comb,
    crecv,
    rsend,
    rrecv,
    rkeep,
    stx,
    tot,
    stz,
    mwt,
    sdt,
    gall,
    sall,
    w_s,
    w_r,
    w_l,
    d_s,
    d_r,
    y_s,
    y_r,
    p_s,
    p_r,
    b_s,
    b_r,
    c_s,
    c_r,
    q_s,
    q_r,
    x_s,
    x_r,
    z_s,
    z_r,
    t_s,
    t_r,
    ag_s,
    ag_r,
    ag_ps,
    ag_pr,
):
    z, x = lax.axis_index("z"), lax.axis_index("x")
    y, c = lax.axis_index("y"), lax.axis_index("c")
    nt = 2 * ny
    nj = ny // 2
    half = xh.shape[1]
    tokens = xh.shape[0]
    par, pairs = y % 2, y // 2
    oc = 1 - c
    yn = y + 1 - 2 * par
    tp = 2 * y + c
    part = nz * ROWS
    quarter = half // 2

    def tile_of(yy, cc):
        return (yy % 2) * nt // 2 + cc * nj + yy // 2

    def tile_at(yy, cc):
        return pl.ds(pl.multiple_of(tile_of(yy, cc) * LANES, LANES), LANES)

    def rows_at(index, size):
        return pl.ds(pl.multiple_of(index * size, size), size)

    def remote(src, dst, send, recv, device):
        return pltpu.make_async_remote_copy(
            src_ref=src,
            dst_ref=dst,
            send_sem=send,
            recv_sem=recv,
            device_id=device,
            device_id_type=MESH,
        )

    def ep_peer(i):
        e = (z * nx + x + i) % (nz * nx)
        return e // nx, e % nx

    def tp_peer(i):
        t = (tp + i) % nt
        return t // 2, t % 2

    barrier = pltpu.get_barrier_semaphore()

    def greet_ep(i, _):
        zz, xx = ep_peer(i)
        pl.semaphore_signal(barrier, inc=1, device_id=(zz, xx, y, c), device_id_type=MESH)
        return _

    def greet_tp(i, _):
        yy, cc = tp_peer(i)
        pl.semaphore_signal(barrier, inc=1, device_id=(z, x, yy, cc), device_id_type=MESH)
        return _

    lax.fori_loop(1, nz * nx, greet_ep, 0)
    lax.fori_loop(1, nt, greet_tp, 0)
    pl.semaphore_wait(barrier, nz * nx - 1 + nt - 1)

    def state_x(i):
        xx = (x + i) % nx
        return remote(state, stx.at[x], x_s.at[i], x_r.at[x], (z, xx, y, c))

    def state_x_from(i):
        xx = (x + i) % nx
        return remote(state, stx.at[xx], x_s.at[i], x_r.at[xx], (z, xx, y, c))

    for i in range(1, nx):
        state_x(i).start()
    stx[x] = state[...]

    def disp_copy(g, zz):
        return remote(
            disp.at[g, rows_at(zz, ROWS)],
            xown.at[g, rows_at(z, ROWS)],
            d_s.at[g, zz],
            d_r.at[g, z],
            (zz, (x + g) % nx, y, c),
        )

    def disp_from(g, zz):
        return remote(
            disp.at[g, rows_at(z, ROWS)],
            xown.at[g, rows_at(zz, ROWS)],
            d_s.at[g, z],
            d_r.at[g, zz],
            (zz, (x + nx - g) % nx, y, c),
        )

    for g in range(nx):
        disp[g] = jnp.dot(
            pick[(x + g) % nx], xh[...], preferred_element_type=jnp.float32
        ).astype(jnp.bfloat16)

        def send(i, _, g=g):
            disp_copy(g, (z + i) % nz).start()
            return _

        lax.fori_loop(1 if g == 0 else 0, nz, send, 0)
    xown[0, rows_at(z, ROWS), :] = disp[0, rows_at(z, ROWS), :]

    width = gate_in.shape[2]
    wcol, wrow = rows_at(c, width), rows_at(c, width)
    moves = (
        (gate_in.at[0], gate.at[:, wcol]),
        (up_in.at[0], up.at[:, wcol]),
        (down_in.at[0], down.at[wrow]),
    )
    swaps = [
        remote(src, dst, w_s.at[k], w_r.at[k], (z, x, y, oc)) for k, (src, dst) in enumerate(moves)
    ]
    ocol, orow = rows_at(oc, width), rows_at(oc, width)
    froms = [
        remote(src, dst, w_s.at[k], w_r.at[k], (z, x, y, oc))
        for k, (src, dst) in enumerate(
            (
                (gate_in.at[0], gate.at[:, ocol]),
                (up_in.at[0], up.at[:, ocol]),
                (down_in.at[0], down.at[orow]),
            )
        )
    ]
    locals_ = [
        pltpu.make_async_copy(src, dst, w_l.at[k]) for k, (src, dst) in enumerate(moves)
    ]
    for copy in swaps + locals_:
        copy.start()

    mrows, srows = mixw.shape[0], shdown.shape[0]

    def tile_copies(i):
        yy, cc = tp_peer(i)
        return (
            remote(
                mixw.at[:, tile_at(yy, cc)],
                mwt.at[rows_at(tp, mrows)],
                t_s.at[0, i],
                t_r.at[0, tp],
                (z, x, yy, cc),
            ),
            remote(
                shdown.at[:, tile_at(yy, cc)],
                sdt.at[rows_at(tp, srows)],
                t_s.at[1, i],
                t_r.at[1, tp],
                (z, x, yy, cc),
            ),
        )

    def tile_from(i):
        yy, cc = tp_peer(i)
        t = 2 * yy + cc
        return (
            remote(
                mixw.at[:, tile_at(y, c)],
                mwt.at[rows_at(t, mrows)],
                t_s.at[0, i],
                t_r.at[0, t],
                (z, x, yy, cc),
            ),
            remote(
                shdown.at[:, tile_at(y, c)],
                sdt.at[rows_at(t, srows)],
                t_s.at[1, i],
                t_r.at[1, t],
                (z, x, yy, cc),
            ),
        )

    def send_tiles(i, _):
        for copy in tile_copies(i):
            copy.start()
        return _

    lax.fori_loop(1, nt, send_tiles, 0)
    mwt[rows_at(tp, mrows), :] = mixw[:, tile_at(y, c)]
    sdt[rows_at(tp, srows), :] = shdown[:, tile_at(y, c)]

    def gather_start(a, piece):
        def go(i, _):
            yy = (y + i) % ny
            remote(
                piece(y, c), piece(y, c), ag_s.at[a, i], ag_r.at[a, y], (z, x, yy, c)
            ).start()
            return _

        lax.fori_loop(1, ny, go, 0)
        remote(piece(y, c), piece(y, c), ag_ps.at[a, y], ag_pr.at[a, y], (z, x, y, oc)).start()

    def gather_forward(a, piece):
        def go(i, _):
            yy = (y + i) % ny
            remote(
                piece(y, c), piece(yy, c), ag_s.at[a, i], ag_r.at[a, yy], (z, x, yy, c)
            ).wait_recv()
            remote(
                piece(yy, c), piece(yy, c), ag_ps.at[a, yy], ag_pr.at[a, yy], (z, x, y, oc)
            ).start()
            return _

        lax.fori_loop(1, ny, go, 0)

    def gather_finish(a, piece):
        def go(yy, _):
            remote(
                piece(yy, c), piece(yy, oc), ag_ps.at[a, yy], ag_pr.at[a, yy], (z, x, y, oc)
            ).wait_recv()
            return _

        lax.fori_loop(0, ny, go, 0)

    def gather_sent(a, piece):
        def go(i, _):
            yy = (y + i) % ny
            remote(
                piece(y, c), piece(y, c), ag_s.at[a, i], ag_r.at[a, y], (z, x, yy, c)
            ).wait_send()
            return _

        def gone(yy, _):
            remote(
                piece(yy, c), piece(yy, c), ag_ps.at[a, yy], ag_pr.at[a, yy], (z, x, y, oc)
            ).wait_send()
            return _

        lax.fori_loop(1, ny, go, 0)
        lax.fori_loop(0, ny, gone, 0)

    arows = act_in.shape[0]
    channels = inside.shape[0]
    gate_piece = lambda yy, cc: gall.at[rows_at(2 * yy + cc, channels)]
    act_piece = lambda yy, cc: sall.at[rows_at(2 * yy + cc, arows)]
    mix_piece = lambda yy, cc: mixer_out.at[:, tile_at(yy, cc)]
    out_piece = lambda yy, cc: expert_out.at[:, tile_at(yy, cc)]

    sall[rows_at(tp, arows), :] = act_in[...]
    gather_start(0, act_piece)

    srow = lax.broadcasted_iota(jnp.int32, (8, KEY_DIM), 0)

    def fold(carry, item):
        mem, st = carry
        mem2, st2 = item[:channels], item[channels:]
        run, run2, dec2 = st[2:3], st2[2:3], st2[1:2]
        new = jnp.maximum(dec2 + run, run2)
        lead, tail = jnp.exp(dec2 + run - new), jnp.exp(run2 - new)
        both = lead * st + tail * st2
        both = jnp.where(srow == 1, st + st2, both)
        both = jnp.where(srow == 2, new, both)
        return lead * mem + tail * mem2, both

    def fresh(run):
        return (
            jnp.zeros((channels, KEY_DIM), jnp.float32),
            jnp.where(srow == 2, run, jnp.zeros((8, KEY_DIM), jnp.float32)),
        )

    for i in range(1, nx):
        state_x_from(i).wait_recv()
    carry = fresh(lowest)
    for i in range(nx):
        carry = fold(carry, stx[i])
    tot[:channels] = carry[0]
    tot[channels:] = carry[1]

    def state_z(zz):
        return remote(tot, stz.at[z], z_s.at[zz], z_r.at[z], (zz, x, y, c))

    def state_z_from(zz):
        return remote(tot, stz.at[zz], z_s.at[z], z_r.at[zz], (zz, x, y, c))

    def send_z(zz, _):
        state_z(zz).start()
        return _

    lax.fori_loop(z + 1, nz, send_z, 0)

    def y_copy(g):
        return remote(xown.at[g], xnbr.at[g], y_s.at[g], y_r.at[g], (z, x, yn, c))

    def p_copy(g):
        return remote(psend.at[g], precv.at[g], p_s.at[g], p_r.at[g], (z, x, yn, c))

    def back_copy(g, zz):
        return remote(
            back.at[g, rows_at(zz, ROWS)],
            rbuf.at[g, rows_at(z, ROWS)],
            b_s.at[g, zz],
            b_r.at[g, z],
            (zz, (x + nx - g) % nx, y, c),
        )

    def back_from(g, zz):
        return remote(
            back.at[g, rows_at(z, ROWS)],
            rbuf.at[g, rows_at(zz, ROWS)],
            b_s.at[g, z],
            b_r.at[g, zz],
            (zz, (x + g) % nx, y, c),
        )

    mine = pl.ds(pl.multiple_of(par * half, half), half)
    other = pl.ds(pl.multiple_of((1 - par) * half, half), half)
    skip = lambda g: jnp.where(g == 0, 1, 0)

    def step(s, acc):
        @pl.when(s < nx)
        def _():
            def wait(i, _):
                disp_from(s, (z + i) % nz).wait_recv()
                return _

            lax.fori_loop(skip(s), nz, wait, 0)
            y_copy(s).start()

        @pl.when(s == 1)
        def _():
            for copy in froms:
                copy.wait_recv()
            for copy in locals_:
                copy.wait()

        @pl.when((s >= 1) & (s <= nx))
        def _():
            g = s - 1
            y_copy(g).wait_recv()
            xa, xb = xown[g], xnbr[g]
            gv = jnp.dot(xa, gate[mine, :], preferred_element_type=jnp.float32)
            gv = gv + jnp.dot(xb, gate[other, :], preferred_element_type=jnp.float32)
            uv = jnp.dot(xa, up[mine, :], preferred_element_type=jnp.float32)
            uv = uv + jnp.dot(xb, up[other, :], preferred_element_type=jnp.float32)
            act = (gv / (1.0 + jnp.exp(-gv)) * uv).astype(jnp.bfloat16)
            psend[g] = jnp.dot(
                act, down[:, other], preferred_element_type=jnp.float32
            ).astype(jnp.bfloat16)
            p_copy(g).start()
            pkeep[g] = jnp.dot(act, down[:, mine], preferred_element_type=jnp.float32)

        @pl.when(s >= 2)
        def _():
            g = s - 2
            p_copy(g).wait_recv()
            back[g] = (pkeep[g] + precv[g].astype(jnp.float32)).astype(jnp.bfloat16)

            def send(i, _):
                back_copy(g, (z + i) % nz).start()
                return _

            lax.fori_loop(skip(g), nz, send, 0)

        return acc

    lax.fori_loop(0, nx + 2, step, 0)
    rbuf[0, rows_at(z, ROWS), :] = back[0, rows_at(z, ROWS), :]

    def from_x(i, carry):
        return fold(carry, stx[i])

    def from_z(zz, carry):
        state_z_from(zz).wait_recv()
        return fold(carry, stz[zz])

    ahead = lax.fori_loop(0, x, from_x, fresh(lowest))
    carry = lax.fori_loop(0, z, from_z, fresh(0.0))
    mem, st = fold(carry, jnp.concatenate(ahead, axis=0))
    across = lax.dot_general(
        jnp.concatenate([mem, st], axis=0),
        scaled[...].astype(jnp.float32),
        (((1,), (1,)), ((), ())),
        precision=lax.Precision.HIGHEST,
        preferred_element_type=jnp.float32,
    )
    carried = rows[0:1] + st[2:3, : rows.shape[1]]
    peak = rows[1:2]
    top = jnp.maximum(carried, peak)
    lead, tail = jnp.exp(carried - top), jnp.exp(peak - top)
    numerator = lead * across[:channels] + tail * inside[...]
    denominator = lead * across[channels : channels + 1] + tail * rows[2:3]
    hidden = numerator / jnp.maximum(jnp.abs(denominator), den_floor)
    gall[rows_at(tp, channels), :] = (hidden * sig[...]).astype(jnp.bfloat16)
    gather_start(1, gate_piece)
    gather_forward(0, act_piece)

    first = True
    for g in range(nx):

        def wait(i, _, g=g):
            back_from(g, (z + i) % nz).wait_recv()
            return _

        lax.fori_loop(1 if g == 0 else 0, nz, wait, 0)
        xx = (x + g) % nx
        dims = (((0,), (0,)), ((), ()))
        got = rbuf[g]
        add = lax.dot_general(whi[xx], got, dims, preferred_element_type=jnp.float32)
        add = add + lax.dot_general(wlo[xx], got, dims, preferred_element_type=jnp.float32)
        comb[...] = add if g == 0 else comb[...] + add
        if g == 0:
            gather_forward(1, gate_piece)

            def wait_tiles(i, _):
                for copy in tile_from(i):
                    copy.wait_recv()
                return _

            lax.fori_loop(1, nt, wait_tiles, 0)
            gather_finish(1, gate_piece)
            mixer_out[:, tile_at(y, c)] = lax.dot_general(
                gall[...], mwt[...], dims, preferred_element_type=jnp.float32
            ).astype(jnp.bfloat16)
            gather_start(2, mix_piece)

    keep = pl.ds(pl.multiple_of(c * quarter, quarter), quarter)
    give = pl.ds(pl.multiple_of(oc * quarter, quarter), quarter)
    core_swap = remote(comb.at[:, give], crecv, c_s, c_r, (z, x, y, oc))
    core_swap.start()
    gather_finish(0, act_piece)
    shared = lax.dot_general(
        sall[...], sdt[...], (((0,), (0,)), ((), ())), preferred_element_type=jnp.float32
    )
    core_swap.wait_recv()
    kept = comb[:, keep] + crecv[...]
    for j in range(nj):
        piece = kept[:, j * LANES : (j + 1) * LANES]
        rkeep[j] = piece
        rsend[j] = piece.astype(jnp.bfloat16)

    def reduce_copy(i):
        j = (pairs + i) % nj
        return remote(
            rsend.at[j], rrecv.at[pairs], q_s.at[i], q_r.at[pairs], (z, x, 2 * j + par, c)
        )

    def reduce_from(i):
        j = (pairs + i) % nj
        return remote(rsend.at[j], rrecv.at[j], q_s.at[i], q_r.at[j], (z, x, 2 * j + par, c))

    for i in range(1, nj):
        reduce_copy(i).start()
    gather_forward(2, mix_piece)
    result = rkeep[pairs] + shared
    for i in range(1, nj):
        reduce_from(i).wait_recv()
        result = result + rrecv[(pairs + i) % nj].astype(jnp.float32)
    expert_out[:, tile_at(y, c)] = result.astype(jnp.bfloat16)
    gather_start(3, out_piece)
    gather_finish(2, mix_piece)
    gather_forward(3, out_piece)
    gather_finish(3, out_piece)

    for i in range(1, nx):
        state_x(i).wait_send()
    for g in range(nx):

        def gone(i, _, g=g):
            zz = (z + i) % nz
            disp_copy(g, zz).wait_send()
            back_copy(g, zz).wait_send()
            return _

        lax.fori_loop(1 if g == 0 else 0, nz, gone, 0)
        y_copy(g).wait_send()
        p_copy(g).wait_send()
    for copy in swaps:
        copy.wait_send()

    def tiles_gone(i, _):
        for copy in tile_copies(i):
            copy.wait_send()
        return _

    def z_gone(zz, _):
        state_z(zz).wait_send()
        return _

    lax.fori_loop(1, nt, tiles_gone, 0)
    lax.fori_loop(z + 1, nz, z_gone, 0)
    core_swap.wait_send()
    for i in range(1, nj):
        reduce_copy(i).wait_send()
    for a, piece in enumerate((act_piece, gate_piece, mix_piece, out_piece)):
        gather_sent(a, piece)


def shards(
    nz,
    nx,
    ny,
    queries,
    key_vectors,
    values,
    out_gate,
    input_gate,
    forget_gate,
    mix_weight,
    expert_input,
    norm_gain,
    route_ids,
    route_weights,
    expert_gate,
    expert_up,
    expert_down,
    shared_gate,
    shared_up,
    shared_down,
):
    y, c = lax.axis_index("y"), lax.axis_index("c")
    tokens, width = expert_input.shape
    half = width // 2
    length = queries.shape[0]
    channels = values.shape[1]
    head = (2 * y + c) // (2 * ny // MEMORY_HEADS)
    state, rows, inside, sig, scaled = mixer_local(
        queries, key_vectors, values, out_gate, input_gate, forget_gate, head
    )
    wide = expert_input.astype(jnp.float32)
    normed = (
        wide
        * lax.rsqrt(jnp.mean(wide * wide, axis=-1, keepdims=True) + epsilon)
        * norm_gain
    ).astype(jnp.bfloat16)
    xh = lax.dynamic_slice_in_dim(normed, (y % 2) * half, half, 1)
    pick, whi, wlo = routing(route_ids, route_weights, y // (ny // 2), c, nz, nx)
    dims = (((0,), (1,)), ((), ()))
    sg = lax.dot_general(shared_gate, normed, dims, preferred_element_type=jnp.float32)
    su = lax.dot_general(shared_up, normed, dims, preferred_element_type=jnp.float32)
    act = (jax.nn.silu(sg) * su).astype(jnp.bfloat16)

    units = expert_gate.shape[2]
    part = nz * ROWS
    nj = ny // 2
    nt = 2 * ny
    vmem = pl.BlockSpec(memory_space=pltpu.VMEM)
    hbm = pl.BlockSpec(memory_space=pl.ANY)
    dma = pltpu.SemaphoreType.DMA
    bf, f32 = jnp.bfloat16, jnp.float32
    return pl.pallas_call(
        functools.partial(kernel, nz, nx, ny),
        out_shape=(
            jax.ShapeDtypeStruct((length, width), bf),
            jax.ShapeDtypeStruct((tokens, width), bf),
        ),
        in_specs=[vmem] * 4 + [hbm] * 3 + [vmem] * 8,
        out_specs=(vmem, vmem),
        scratch_shapes=[
            pltpu.VMEM((width, 2 * units), bf),
            pltpu.VMEM((width, 2 * units), bf),
            pltpu.VMEM((2 * units, width), bf),
            pltpu.VMEM((nx, part, half), bf),
            pltpu.VMEM((nx, part, half), bf),
            pltpu.VMEM((nx, part, half), bf),
            pltpu.VMEM((nx, part, half), f32),
            pltpu.VMEM((nx, part, half), bf),
            pltpu.VMEM((nx, part, half), bf),
            pltpu.VMEM((nx, part, half), bf),
            pltpu.VMEM((nx, part, half), bf),
            pltpu.VMEM((tokens, half), f32),
            pltpu.VMEM((tokens, half // 2), f32),
            pltpu.VMEM((nj, tokens, LANES), bf),
            pltpu.VMEM((nj, tokens, LANES), bf),
            pltpu.VMEM((nj, tokens, LANES), f32),
            pltpu.VMEM((nx, channels + 8, KEY_DIM), f32),
            pltpu.VMEM((channels + 8, KEY_DIM), f32),
            pltpu.VMEM((nz, channels + 8, KEY_DIM), f32),
            pltpu.VMEM((nt * channels, LANES), bf),
            pltpu.VMEM((nt * shared_down.shape[0], LANES), bf),
            pltpu.VMEM((nt * channels, length), bf),
            pltpu.VMEM((nt * shared_down.shape[0], tokens), bf),
            dma((3,)),
            dma((3,)),
            dma((3,)),
            dma((nx, nz)),
            dma((nx, nz)),
            dma((nx,)),
            dma((nx,)),
            dma((nx,)),
            dma((nx,)),
            dma((nx, nz)),
            dma((nx, nz)),
            dma,
            dma,
            dma((nj,)),
            dma((nj,)),
            dma((nx,)),
            dma((nx,)),
            dma((nz,)),
            dma((nz,)),
            dma((2, nt)),
            dma((2, nt)),
            dma((4, ny)),
            dma((4, ny)),
            dma((4, ny)),
            dma((4, ny)),
        ],
        compiler_params=pltpu.CompilerParams(
            collective_id=0, has_side_effects=True, vmem_limit_bytes=50 * 1024 * 1024
        ),
        name="exchange",
    )(
        xh,
        pick,
        whi,
        wlo,
        expert_gate,
        expert_up,
        expert_down,
        state,
        rows,
        inside,
        sig,
        scaled,
        mix_weight,
        act,
        shared_down,
    )


def solution(mesh):
    count, nt = mesh.shape["ep"], mesh.shape["tp"]
    nx = 4 if count % 16 == 0 else 2
    nz, ny = count // nx, nt // 2
    finer = Mesh(mesh.devices.reshape(nz, nx, ny, 2), ("z", "x", "y", "c"))
    placed = (
        P(EP, None),
        P(EP, None),
        P(EP, TP),
        P(EP, TP),
        P(EP, None),
        P(EP, None),
        P(TP, None),
        P(EP, None),
        P(),
        P(EP, None),
        P(EP, None),
        P(EP + TP, None, None),
        P(EP + TP, None, None),
        P(EP + TP, None, None),
        P(None, TP),
        P(None, TP),
        P(TP, None),
    )
    return jax.shard_map(
        functools.partial(shards, nz, nx, ny),
        mesh=finer,
        in_specs=placed,
        out_specs=(P(EP, None), P(EP, None)),
        check_vma=False,
    )
```
